32 devices in a mesh: sp: 16 (over z, y, x), tp: 2 (over core).
Axes of the slice: x: 2, y: 2, z: 4, core: 2. Of those that a mesh axis runs over, the one named last changes fastest.
Arguments:
- proj_a: bfloat16 [4096, 3072], P('sp', 'tp'), may hold values from -20 to 20
- proj_gate: bfloat16 [4096, 3072], P('sp', 'tp'), may hold values from -6 to 6
- taps: bfloat16 [31, 3072], P(None, 'tp'), may hold values from -1 to 1
- norm_gain: float32 [3072], P('tp'), may hold values from 0.1 to 1.9
- norm_shift: float32 [3072], P('tp'), may hold values from -3 to 3
- cotangent: bfloat16 [4096, 3072], P('sp', 'tp'), may hold values from -6 to 6
Outputs:
- a_grad: bfloat16 [4096, 3072], P('sp', 'tp')
- gate_grad: bfloat16 [4096, 3072], P('sp', 'tp')
- taps_grad: float32 [31, 3072], P(None, 'tp')
- gain_grad: float32 [3072], P('tp')
- shift_grad: float32 [3072], P('tp')
The draws below stay inside these ranges and needn't reach their ends.
All inputs are finite; a program needn't handle non-finite values.
Results may differ from the reference program's by a relative error of at most 0.0048.
Values may be sent and summed in bfloat16 or wider, within the bound.
A program may use at most 64 MiB of HBM per device.

```python
import jax
import jax.numpy as jnp
from jax import lax

D = 3072
K = 31
TOK_DEV = 256
TOKENS = 4096
N_SP = 16


def draw_proj_a(key, part):
    first_key, second_key, third_key = jax.random.split(jax.random.fold_in(key, 17), 3)
    groups = jnp.arange(D) * 24 // D
    factors = jnp.exp(jax.random.uniform(second_key, (24,), jnp.float32, -1.1, 1.1))
    col_scale = factors[groups]
    row_groups = jnp.arange(TOKENS) * 64 // TOKENS
    row_factors = jnp.exp(jax.random.uniform(third_key, (64,), jnp.float32, -0.5, 0.5))
    row_scale = row_factors[row_groups]
    base = jax.random.truncated_normal(first_key, -4.0, 4.0, (TOKENS, D), jnp.float32)
    return (base * col_scale[None, :] * row_scale[:, None]).astype(jnp.bfloat16)


def level_of(own_key, dims, cuts, least, high):
    factor_of, own = 1.0, jax.random.fold_in(own_key, 6)
    for axis_at, parts in cuts:
        steps = jnp.exp(jax.random.uniform(jax.random.fold_in(own, axis_at), (parts,), jnp.float32, least / len(cuts), high / len(cuts)))
        factor_of = factor_of * jnp.repeat(steps, dims[axis_at] // parts).reshape([-1 if axis == axis_at else 1 for axis in range(len(dims))])
    return factor_of


def centred(key, extent, scale, most, shards=(), kind=jnp.bfloat16):
    entries = scale * jax.random.normal(key, extent, jnp.float32)
    if shards:
        entries = entries * level_of(key, extent, shards, -0.22, 0.18)
    return jnp.clip(entries, -most, most).astype(kind)


def setup_inputs(seed: int = 0) -> dict:
    key_of = jax.random.split(jax.random.key(seed), 7)
    return {
        "proj_a": draw_proj_a(jax.random.fold_in(key_of[6], 71), 0),
        "proj_gate": centred(key_of[1], (TOKENS, D), 1.5, 6.0, ((0, 16), (1, 2))),
        "taps": centred(key_of[2], (K, D), K ** -0.5, 1.0, ((1, 2),)),
        "norm_gain": jnp.clip(1.0 + 0.18 * jax.random.normal(key_of[3], (D,), jnp.float32), 0.1, 1.9),
        "norm_shift": centred(key_of[4], (D,), 0.5, 3.0, ((0, 2),), jnp.float32),
        "cotangent": centred(key_of[5], (TOKENS, D), 1.0, 6.0, ((0, 16), (1, 2))),
    }


EPS = 1e-05

def reference(proj_a, proj_gate, taps, norm_gain, norm_shift, cotangent):
    width = taps.shape[0]
    edge = width - 1
    rows = TOK_DEV
    blocks = N_SP
    gate_f = proj_gate.astype(jnp.float32)
    glu = (proj_a.astype(jnp.float32) * jax.nn.sigmoid(gate_f)).astype(jnp.bfloat16)
    glu_pad = jnp.concatenate([jnp.zeros((edge, D), jnp.bfloat16), glu], axis=0)
    tapf = taps.astype(jnp.float32)
    gain = norm_gain.astype(jnp.float32)
    shift = norm_shift.astype(jnp.float32)

    def first(index):
        start = index * rows
        ext = lax.dynamic_slice_in_dim(glu_pad, start, rows + edge, 0).astype(jnp.float32)
        cot = lax.dynamic_slice_in_dim(cotangent, start, rows, 0).astype(jnp.float32)
        conv = jnp.zeros((rows, D), jnp.float32)
        for k in range(width):
            conv = conv + tapf[k] * ext[k:k + rows]
        mean = lax.optimization_barrier(jnp.mean(conv, axis=1, keepdims=True))
        cent = conv - mean
        spread = lax.optimization_barrier(jnp.mean(cent * cent, axis=1, keepdims=True))
        rstd = lax.rsqrt(spread + EPS)
        normed = cent * rstd
        pre = normed * gain + shift
        sig = jax.nn.sigmoid(pre)
        dpre = cot * sig * (1.0 + pre * (1.0 - sig))
        dnormed = dpre * gain
        dconv = rstd * (dnormed - lax.optimization_barrier(jnp.mean(dnormed, axis=1, keepdims=True)) - normed * lax.optimization_barrier(jnp.mean(dnormed * normed, axis=1, keepdims=True)))
        return (dconv, lax.optimization_barrier(jnp.sum(dpre * normed, axis=0)), lax.optimization_barrier(jnp.sum(dpre, axis=0)))
    index = jnp.arange(blocks, dtype=jnp.int32)
    dconv_all, gain_parts, shift_parts = lax.map(first, index)
    dconv_pad = jnp.concatenate([dconv_all.reshape(blocks * rows, D), jnp.zeros((edge, D), jnp.float32)], axis=0)

    def second(index):
        start = index * rows
        dext = lax.dynamic_slice_in_dim(dconv_pad, start, rows + edge, 0)
        ext = lax.dynamic_slice_in_dim(glu_pad, start, rows + edge, 0).astype(jnp.float32)
        own = dext[:rows]
        dglu = jnp.zeros((rows, D), jnp.float32)
        for k in range(width):
            dglu = dglu + tapf[edge - k] * dext[k:k + rows]
        taps_part = jnp.stack([lax.optimization_barrier(jnp.sum(own * ext[j:j + rows], axis=0)) for j in range(width)])
        a_rows = lax.dynamic_slice_in_dim(proj_a, start, rows, 0).astype(jnp.float32)
        g_rows = lax.dynamic_slice_in_dim(gate_f, start, rows, 0)
        sg = jax.nn.sigmoid(g_rows)
        return ((dglu * sg).astype(jnp.bfloat16), (dglu * a_rows * sg * (1.0 - sg)).astype(jnp.bfloat16), taps_part)
    a_parts, gate_parts, taps_parts = lax.map(second, index)
    a_grad = a_parts.reshape(blocks * rows, D)
    gate_grad = gate_parts.reshape(blocks * rows, D)
    return (a_grad, gate_grad, lax.optimization_barrier(jnp.sum(taps_parts, axis=0)), lax.optimization_barrier(jnp.sum(gain_parts, axis=0)), lax.optimization_barrier(jnp.sum(shift_parts, axis=0)))
```

```python
import functools

import jax
import jax.numpy as jnp
from jax import lax
from jax.experimental import pallas as pl
from jax.experimental.pallas import tpu as pltpu
from jax.sharding import PartitionSpec as P

EPS = 1e-05
LANES = 128
SUB = 8
PACK = 16
BLOCK = 64
HALO = 32
STEP = SUB + 1
F32 = jnp.float32
BF16 = jnp.bfloat16


def plan(chans, width, n):
    tiles = chans // LANES
    rounds = 2 if tiles % 2 == 0 else 1
    slots = -(-(width + 1) // SUB) * SUB
    total = tiles // rounds * (slots + 1)
    share = PACK * max(n // 2, 1)
    chunk = -(-total // share) * PACK
    owners = -(-total // chunk)
    return tiles, rounds, slots, chunk, owners, (n - owners) // 2


def products(pairs):
    total = None
    for x, y in pairs:
        prod = x.astype(F32) * y.astype(F32)
        total = prod if total is None else total + prod
    return total


def kernel(
    n, width, full,
    a_hbm, g_hbm, taps_hbm, gain_hbm, shift_hbm, cot_hbm,
    ag_ref, gg_ref, sums_ref,
    a_ref, g_ref, cot_ref, taps_ref, gain_ref, shift_ref,
    tap_s, x_s, xa_s, xb_s, conv_s, dn_s, d_s, d_t, da_s, db_s, par_s, part_s,
    glu_out, glu_in, dc_out, dc_in,
    st_out, st_in, stat_s,
    red_f, red_s, rs_in, ag_src, ag_in,
    in_sem, halo_send, halo_recv, st_send, st_recv,
    rs_send, rs_recv, ag_send, ag_recv,
):
    rows, chans = a_hbm.shape
    edge = width - 1
    lead = HALO - edge
    tiles, rounds, slots, chunk, owners, first_owner = plan(chans, width, n)
    part_tiles = tiles // rounds
    blocks = rows // BLOCK
    far, near = (rows - BLOCK) // PACK, BLOCK // PACK
    loads = [
        pltpu.make_async_copy(src, dst, in_sem.at[i])
        for i, (src, dst) in enumerate((
            (taps_hbm, taps_ref),
            (g_hbm, g_ref),
            (a_hbm, a_ref),
            (gain_hbm, gain_ref),
            (shift_hbm, shift_ref),
            (cot_hbm, cot_ref),
        ))
    ]
    for load in loads:
        load.start()
    me = lax.axis_index("sp")
    other = 1 - lax.axis_index("tp")

    barrier = pltpu.get_barrier_semaphore()

    def greet(step, carry):
        pl.semaphore_signal(barrier, inc=1, device_id={"sp": lax.rem(me + step, n)})
        return carry

    pl.semaphore_signal(barrier, inc=1, device_id={"tp": other})
    lax.fori_loop(1, n, greet, 0)

    def cols(j):
        return pl.ds(pl.multiple_of(j * LANES, LANES), LANES)

    def each_tile(run):
        def step(j, carry):
            run(j)
            return carry

        lax.fori_loop(0, tiles, step, 0)

    def over_tiles(run, carry, unroll):
        unroll = unroll if tiles % unroll == 0 else 1

        def step(i, carry):
            for u in range(unroll):
                carry = run(i * unroll + u, carry)
            return carry

        return lax.fori_loop(0, tiles // unroll, step, carry)

    glu_copy = pltpu.make_async_remote_copy(
        src_ref=glu_out, dst_ref=glu_in, send_sem=halo_send.at[0], recv_sem=halo_recv.at[0],
        device_id={"sp": lax.rem(me + 1, n)},
    )
    dc_copy = pltpu.make_async_remote_copy(
        src_ref=dc_out, dst_ref=dc_in, send_sem=halo_send.at[1], recv_sem=halo_recv.at[1],
        device_id={"sp": lax.rem(me + n - 1, n)},
    )

    def spread(src, dst, j, base, stride, count, at=0):
        for m in range(count):
            dst[j, at + m] = src[j, pl.ds(base + m, PACK, stride=stride), :].astype(BF16)

    def correlate(src, dst, j, base, stride, order):
        for m in range(stride):
            dst[j, pl.ds(base + m, PACK, stride=stride), :] = products(
                (src[j, m + i], tap_s[j, k]) for i, k in enumerate(order)
            )

    forward = range(width)
    backward = range(edge, -1, -1)

    def spread_taps(j):
        for k in range(width):
            row = taps_ref[pl.ds(k, 1), cols(j)].astype(F32)
            tap_s[j, k] = jnp.broadcast_to(row, (PACK, LANES)).astype(BF16)

    def gate_tile(j):
        for b in range(blocks):
            at = pl.ds(b * BLOCK, BLOCK)
            a = a_ref[at, cols(j)].astype(F32)
            g = g_ref[at, cols(j)].astype(F32)
            glu = (a * jax.nn.sigmoid(g)).astype(BF16)
            x_s[j, pl.ds(HALO + b * BLOCK, BLOCK), :] = glu.astype(F32)
            if b == blocks - 1:
                glu_out[j] = glu[BLOCK - HALO :]
        spread(x_s, xa_s, j, lead + BLOCK, far, far + edge)

    loads[0].wait()
    each_tile(spread_taps)
    loads[1].wait()
    loads[2].wait()
    each_tile(gate_tile)
    pl.semaphore_wait(barrier, n)

    @pl.when(me < n - 1)
    def _():
        glu_copy.start()

    each_tile(lambda j: correlate(xa_s, conv_s, j, BLOCK, far, forward))

    lane = lax.broadcasted_iota(jnp.int32, (BLOCK, LANES), 1)
    zero = jnp.zeros((BLOCK, LANES), F32)

    def stat_copy(i):
        return pltpu.make_async_remote_copy(
            src_ref=st_out.at[i], dst_ref=st_in.at[i], send_sem=st_send.at[i],
            recv_sem=st_recv.at[i], device_id={"tp": other},
        )

    def send_stats(i, first, second):
        first = jnp.sum(first, axis=1, keepdims=True)
        second = jnp.sum(second, axis=1, keepdims=True)
        st_out[i] = jnp.where(lane < LANES // 2, first, second)
        stat_copy(i).start()

    def both_stats(i):
        stat_copy(i).wait_recv()
        both = (st_out[i] + st_in[i]) * (1.0 / full)
        first = jnp.broadcast_to(both[:, 0:1], (BLOCK, LANES))
        second = jnp.broadcast_to(both[:, LANES // 2 : LANES // 2 + 1], (BLOCK, LANES))
        return first, second

    def moments(b):
        def step(j, carry):
            first, second = carry
            x = conv_s[j, pl.ds(b * BLOCK, BLOCK), :]
            return first + x, second + x * x

        send_stats(b, *over_tiles(step, (zero, zero), 3))

    def fold(x):
        return jnp.sum(x.reshape(x.shape[0] // SUB, SUB, LANES), axis=0)

    def normalise(b):
        at = pl.ds(b * BLOCK, BLOCK)
        mean, square = both_stats(b)
        rstd = lax.rsqrt(jnp.maximum(square - mean * mean, 0.0) + EPS)
        stat_s[at, :] = rstd

        def step(j, carry):
            first, second = carry
            gain = par_s[j, 0:1, :]
            normed = (conv_s[j, at, :] - mean) * rstd
            pre = normed * gain + par_s[j, 1:2, :]
            sig = jax.nn.sigmoid(pre)
            dpre = cot_ref[at, cols(j)].astype(F32) * sig * (1.0 + pre * (1.0 - sig))
            par_s[j, pl.ds(SUB, SUB), :] += fold(dpre * normed)
            par_s[j, pl.ds(2 * SUB, SUB), :] += fold(dpre)
            dn = dpre * gain
            conv_s[j, at, :] = normed
            dn_s[j, at, :] = dn
            return first + dn, second + dn * normed

        send_stats(blocks + b, *lax.fori_loop(0, tiles, step, (zero, zero)))

    def dconv(b):
        at = pl.ds(b * BLOCK, BLOCK)
        first, second = both_stats(blocks + b)
        rstd = stat_s[at, :]

        def step(j, carry):
            d_s[j, at, :] = rstd * (dn_s[j, at, :] - first - conv_s[j, at, :] * second)
            return carry

        over_tiles(step, 0, 2)

    for b in range(1, blocks):
        moments(b)

    loads[3].wait()
    loads[4].wait()

    def parameters(j):
        par_s[j, 0:1, :] = gain_ref[cols(j)].reshape(1, LANES)
        par_s[j, 1:2, :] = shift_ref[cols(j)].reshape(1, LANES)
        par_s[j, pl.ds(SUB, 2 * SUB), :] = jnp.zeros((2 * SUB, LANES), F32)

    each_tile(parameters)
    loads[5].wait()

    @pl.when(me > 0)
    def _():
        glu_copy.wait_recv()

        def widen(j):
            x_s[j, pl.ds(0, HALO), :] = glu_in[j].astype(F32)

        each_tile(widen)

    @pl.when(me == 0)
    def _():
        def clear(j):
            x_s[j, pl.ds(0, HALO), :] = jnp.zeros((HALO, LANES), F32)

        each_tile(clear)

    def near_tile(j):
        spread(x_s, xb_s, j, lead, near, near + edge)
        correlate(xb_s, conv_s, j, 0, near, forward)

    each_tile(near_tile)
    moments(0)
    order = (*range(1, blocks), 0)
    for b in order:
        normalise(b)
    for b in order:
        dconv(b)

    def head(j):
        dc_out[j] = d_s[j, pl.ds(0, HALO), :].astype(BF16)

    each_tile(head)

    @pl.when(me > 0)
    def _():
        dc_copy.start()

    spare = owners * chunk - part_tiles * (slots + 1)
    part_s[pl.ds(width * STEP, (slots - width) * STEP), :] = jnp.zeros(
        ((slots - width) * STEP, LANES), F32
    )

    def taps_round(h):
        def step(i, carry):
            j = h * part_tiles + i
            spread(d_s, d_t, j, BLOCK, far, far)
            spread(d_s, d_t, j, 0, near, near, far)
            for k in range(width):
                both = products(
                    [(xa_s[j, m + k], d_t[j, m]) for m in range(far)]
                    + [(xb_s[j, m + k], d_t[j, far + m]) for m in range(near)]
                )
                part_s[pl.ds(k * STEP, SUB), :] = both[:SUB] + both[SUB:]
            part_s[pl.ds(width * STEP, SUB), :] = par_s[j, pl.ds(SUB, SUB), :]
            for q in range(slots // SUB):
                total = part_s[pl.ds(q * SUB * STEP, SUB, stride=STEP), :]
                for r in range(1, SUB):
                    total = total + part_s[pl.ds(q * SUB * STEP + r, SUB, stride=STEP), :]
                red_f[pl.ds(pl.multiple_of(i * slots, SUB) + q * SUB, SUB), :] = total
            red_f[pl.ds(part_tiles * slots + i, 1), :] = jnp.sum(
                par_s[j, pl.ds(2 * SUB, SUB), :], axis=0, keepdims=True
            )
            return carry

        lax.fori_loop(0, part_tiles, step, 0)
        if spare:
            red_f[pl.ds(part_tiles * (slots + 1), spare), :] = jnp.zeros((spare, LANES), F32)
        red_s[h] = red_f[...].astype(BF16)

    mine = me - first_owner
    owner = jnp.logical_and(mine >= 0, mine < owners)

    def part(o):
        return pl.ds(pl.multiple_of(o * chunk, PACK), chunk)

    def bytes_of(ref, sem):
        return pltpu.make_async_copy(ref, ref, sem)

    def scatter(h):
        def step(i, carry):
            o = lax.rem(me + i, owners)
            to = first_owner + o

            @pl.when(to != me)
            def _():
                pltpu.make_async_remote_copy(
                    src_ref=red_s.at[h, part(o), :],
                    dst_ref=rs_in.at[h, lax.rem(me - to + n, n) - 1],
                    send_sem=rs_send.at[h], recv_sem=rs_recv.at[h], device_id={"sp": to},
                ).start()

            return carry

        lax.fori_loop(0, owners, step, 0)

    def gather(h):
        @pl.when(owner)
        def _():
            bytes_of(rs_in.at[h], rs_recv.at[h]).wait()
            ag_src[h] = lax.fori_loop(
                0, n - 1, lambda s, total: total + rs_in[h, s].astype(F32),
                red_s[h, part(mine), :].astype(F32),
            ).astype(BF16)

            def step(i, carry):
                pltpu.make_async_remote_copy(
                    src_ref=ag_src.at[h], dst_ref=ag_in.at[h, part(mine), :],
                    send_sem=ag_send.at[h], recv_sem=ag_recv.at[h],
                    device_id={"sp": lax.rem(me + i, n)},
                ).start()
                return carry

            lax.fori_loop(1, n, step, 0)

    for h in range(rounds):
        taps_round(h)
        scatter(h)

    def back_far(j):
        spread(d_s, da_s, j, 0, far, far + edge)
        correlate(da_s, x_s, j, 0, far, backward)

    def back_near(j):
        spread(d_s, db_s, j, rows - BLOCK, near, near + edge)
        correlate(db_s, x_s, j, rows - BLOCK, near, backward)

    def outputs(b):
        at = pl.ds(b * BLOCK, BLOCK)

        def run(j):
            sig = jax.nn.sigmoid(g_ref[at, cols(j)].astype(F32))
            first = x_s[j, at, :] * sig
            ag_ref[at, cols(j)] = first.astype(BF16)
            gg_ref[at, cols(j)] = (first * a_ref[at, cols(j)].astype(F32) * (1.0 - sig)).astype(BF16)

        each_tile(run)

    each_tile(back_far)
    for b in range(blocks - 1):
        outputs(b)
    for h in range(rounds):
        gather(h)

    @pl.when(me < n - 1)
    def _():
        dc_copy.wait_recv()

        def widen(j):
            d_s[j, pl.ds(rows, HALO), :] = dc_in[j].astype(F32)

        each_tile(widen)

    @pl.when(me == n - 1)
    def _():
        def clear(j):
            d_s[j, pl.ds(rows, HALO), :] = jnp.zeros((HALO, LANES), F32)

        each_tile(clear)

    each_tile(back_near)
    outputs(blocks - 1)

    @pl.when(me < n - 1)
    def _():
        glu_copy.wait_send()

    @pl.when(me > 0)
    def _():
        dc_copy.wait_send()

    for i in range(2 * blocks):
        stat_copy(i).wait_send()

    for h in range(rounds):
        @pl.when(owner)
        def _():
            bytes_of(rs_in.at[h], ag_send.at[h]).wait()
            if owners > 1:
                rest = pl.ds(0, (owners - 1) * chunk)
                bytes_of(red_s.at[h, rest, :], rs_send.at[h]).wait()
                bytes_of(ag_in.at[h, rest, :], ag_recv.at[h]).wait()
            ag_in[h, part(mine), :] = ag_src[h]

        @pl.when(jnp.logical_not(owner))
        def _():
            bytes_of(red_s.at[h], rs_send.at[h]).wait()
            bytes_of(ag_in.at[h], ag_recv.at[h]).wait()

        sums_ref[h] = ag_in[h].astype(F32)


def finish(
    width, slots, part_tiles,
    ag_ref, gg_ref, sums_ref,
    ag_out, gg_out, tg_out, gaing_out, shiftg_out,
    tg_ref, gaing_ref, shiftg_ref, sems,
):
    copies = [
        pltpu.make_async_copy(src, dst, sems.at[i])
        for i, (src, dst) in enumerate((
            (ag_ref, ag_out), (gg_ref, gg_out), (tg_ref, tg_out),
            (gaing_ref, gaing_out), (shiftg_ref, shiftg_out),
        ))
    ]
    copies[0].start()
    copies[1].start()
    for h in range(sums_ref.shape[0]):
        for i in range(part_tiles):
            at = pl.ds((h * part_tiles + i) * LANES, LANES)
            tg_ref[:, at] = sums_ref[h, pl.ds(i * slots, width), :]
            gaing_ref[at] = sums_ref[h, i * slots + width, :]
            shiftg_ref[at] = sums_ref[h, part_tiles * slots + i, :]
    for copy in copies[2:]:
        copy.start()
    for copy in copies:
        copy.wait()


def solution(mesh):
    n, ntp = mesh.shape["sp"], mesh.shape["tp"]

    def body(proj_a, proj_gate, taps, norm_gain, norm_shift, cotangent):
        rows, chans = proj_a.shape
        width = taps.shape[0]
        edge = width - 1
        tiles, rounds, slots, chunk, owners, _ = plan(chans, width, n)
        blocks = rows // BLOCK
        far, near = (rows - BLOCK) // PACK, BLOCK // PACK
        vmem = pl.BlockSpec(memory_space=pltpu.VMEM)
        hbm = pl.BlockSpec(memory_space=pltpu.HBM)
        wide = jax.ShapeDtypeStruct((rows, chans), BF16)
        a_grad, gate_grad, sums = pl.pallas_call(
            functools.partial(kernel, n, width, chans * ntp),
            out_shape=(wide, wide, jax.ShapeDtypeStruct((rounds, owners * chunk, LANES), F32)),
            in_specs=[hbm] * 6,
            out_specs=(vmem,) * 3,
            scratch_shapes=[
                pltpu.VMEM((rows, chans), BF16),
                pltpu.VMEM((rows, chans), BF16),
                pltpu.VMEM((rows, chans), BF16),
                pltpu.VMEM((width, chans), BF16),
                pltpu.VMEM((chans,), F32),
                pltpu.VMEM((chans,), F32),
                pltpu.VMEM((tiles, width, PACK, LANES), BF16),
                pltpu.VMEM((tiles, HALO + rows, LANES), F32),
                pltpu.VMEM((tiles, far + edge, PACK, LANES), BF16),
                pltpu.VMEM((tiles, near + edge, PACK, LANES), BF16),
                pltpu.VMEM((tiles, rows, LANES), F32),
                pltpu.VMEM((tiles, rows, LANES), F32),
                pltpu.VMEM((tiles, rows + HALO, LANES), F32),
                pltpu.VMEM((tiles, far + near, PACK, LANES), BF16),
                pltpu.VMEM((tiles, far + edge, PACK, LANES), BF16),
                pltpu.VMEM((tiles, near + edge, PACK, LANES), BF16),
                pltpu.VMEM((tiles, 3 * SUB, LANES), F32),
                pltpu.VMEM((slots * STEP, LANES), F32),
                pltpu.VMEM((tiles, HALO, LANES), BF16),
                pltpu.VMEM((tiles, HALO, LANES), BF16),
                pltpu.VMEM((tiles, HALO, LANES), BF16),
                pltpu.VMEM((tiles, HALO, LANES), BF16),
                pltpu.VMEM((2 * blocks, BLOCK, LANES), F32),
                pltpu.VMEM((2 * blocks, BLOCK, LANES), F32),
                pltpu.VMEM((rows, LANES), F32),
                pltpu.VMEM((owners * chunk, LANES), F32),
                pltpu.VMEM((rounds, owners * chunk, LANES), BF16),
                pltpu.VMEM((rounds, n - 1, chunk, LANES), BF16),
                pltpu.VMEM((rounds, chunk, LANES), BF16),
                pltpu.VMEM((rounds, owners * chunk, LANES), BF16),
                pltpu.SemaphoreType.DMA((6,)),
                pltpu.SemaphoreType.DMA((2,)),
                pltpu.SemaphoreType.DMA((2,)),
                pltpu.SemaphoreType.DMA((2 * blocks,)),
                pltpu.SemaphoreType.DMA((2 * blocks,)),
                pltpu.SemaphoreType.DMA((rounds,)),
                pltpu.SemaphoreType.DMA((rounds,)),
                pltpu.SemaphoreType.DMA((rounds,)),
                pltpu.SemaphoreType.DMA((rounds,)),
            ],
            compiler_params=pltpu.CompilerParams(
                collective_id=0, has_side_effects=True, vmem_limit_bytes=40 * 1024 * 1024
            ),
        )(*(
            pltpu.with_memory_space_constraint(x, pltpu.HBM)
            for x in (proj_a, proj_gate, taps, norm_gain, norm_shift, cotangent)
        ))
        vector = jax.ShapeDtypeStruct((chans,), F32)
        return pl.pallas_call(
            functools.partial(finish, width, slots, tiles // rounds),
            out_shape=(wide, wide, jax.ShapeDtypeStruct((width, chans), F32), vector, vector),
            in_specs=[vmem] * 3,
            out_specs=(hbm,) * 5,
            scratch_shapes=[
                pltpu.VMEM((width, chans), F32),
                pltpu.VMEM((chans,), F32),
                pltpu.VMEM((chans,), F32),
                pltpu.SemaphoreType.DMA((5,)),
            ],
            compiler_params=pltpu.CompilerParams(vmem_limit_bytes=16 * 1024 * 1024),
        )(a_grad, gate_grad, sums)

    placed = (P("sp", "tp"), P("sp", "tp"), P(None, "tp"), P("tp"), P("tp"), P("sp", "tp"))
    return jax.shard_map(
        body,
        mesh=mesh,
        in_specs=placed,
        out_specs=(P("sp", "tp"), P("sp", "tp"), P(None, "tp"), P("tp"), P("tp")),
        check_vma=False,
    )
```

```python
import functools

import jax
import jax.numpy as jnp
from jax import lax
from jax.experimental import pallas as pl
from jax.experimental.pallas import tpu as pltpu
from jax.sharding import PartitionSpec as P

EPS = 1e-05
LANES = 128
SUB = 8
PACK = 16
BLOCK = 64
HALO = 32
STEP = SUB + 1
F32 = jnp.float32
BF16 = jnp.bfloat16


def plan(chans, width, n):
    tiles = chans // LANES
    rounds = 2 if tiles % 2 == 0 else 1
    slots = -(-(width + 1) // SUB) * SUB
    total = tiles // rounds * (slots + 1)
    share = PACK * max(n // 2, 1)
    chunk = -(-total // share) * PACK
    owners = -(-total // chunk)
    return tiles, rounds, slots, chunk, owners, (n - owners) // 2


def products(pairs):
    total = None
    for x, y in pairs:
        prod = x.astype(F32) * y.astype(F32)
        total = prod if total is None else total + prod
    return total


def kernel(
    n, width, full,
    a_hbm, g_hbm, taps_hbm, gain_hbm, shift_hbm, cot_hbm,
    ag_ref, gg_ref, sums_ref,
    a_ref, g_ref, cot_ref, taps_ref, gain_ref, shift_ref,
    tap_s, x_s, xa_s, xb_s, conv_s, dn_s, d_s, d_t, da_s, db_s, par_s, part_s,
    glu_out, glu_in, dc_out, dc_in,
    st_out, st_in, stat_s,
    red_f, red_s, rs_in, ag_src, ag_in,
    in_sem, halo_send, halo_recv, st_send, st_recv,
    rs_send, rs_recv, ag_send, ag_recv,
):
    rows, chans = a_hbm.shape
    edge = width - 1
    lead = HALO - edge
    tiles, rounds, slots, chunk, owners, first_owner = plan(chans, width, n)
    part_tiles = tiles // rounds
    far, near = (rows - HALO) // PACK, HALO // PACK
    first_rows = (0, HALO)
    late = ((HALO, BLOCK - HALO), *((b, BLOCK) for b in range(BLOCK, rows, BLOCK)))
    parts = 2 if tiles % 2 == 0 else 1
    split = tiles // parts
    halves = [pl.ds(h * split * LANES, split * LANES) for h in range(parts)]
    pieces = [(taps_hbm, taps_ref)]
    for half in halves:
        pieces += [(g_hbm.at[:, half], g_ref.at[:, half]), (a_hbm.at[:, half], a_ref.at[:, half])]
    pieces += [(gain_hbm, gain_ref), (shift_hbm, shift_ref), (cot_hbm, cot_ref)]
    loads = [
        pltpu.make_async_copy(src, dst, in_sem.at[i]) for i, (src, dst) in enumerate(pieces)
    ]
    for load in loads:
        load.start()
    me = lax.axis_index("sp")
    other = 1 - lax.axis_index("tp")

    barrier = pltpu.get_barrier_semaphore()

    def greet(step, carry):
        pl.semaphore_signal(barrier, inc=1, device_id={"sp": lax.rem(me + step, n)})
        return carry

    pl.semaphore_signal(barrier, inc=1, device_id={"tp": other})
    lax.fori_loop(1, n, greet, 0)

    def cols(j):
        return pl.ds(pl.multiple_of(j * LANES, LANES), LANES)

    def each_tile(run):
        def step(j, carry):
            run(j)
            return carry

        lax.fori_loop(0, tiles, step, 0)

    def over_tiles(run, carry, unroll):
        unroll = unroll if tiles % unroll == 0 else 1

        def step(i, carry):
            for u in range(unroll):
                carry = run(i * unroll + u, carry)
            return carry

        return lax.fori_loop(0, tiles // unroll, step, carry)

    glu_copy = pltpu.make_async_remote_copy(
        src_ref=glu_out, dst_ref=glu_in, send_sem=halo_send.at[0], recv_sem=halo_recv.at[0],
        device_id={"sp": lax.rem(me + 1, n)},
    )
    dc_copy = pltpu.make_async_remote_copy(
        src_ref=dc_out, dst_ref=dc_in, send_sem=halo_send.at[1], recv_sem=halo_recv.at[1],
        device_id={"sp": lax.rem(me + n - 1, n)},
    )

    def spread(src, dst, j, base, stride, count):
        for m in range(count):
            dst[j, m] = src[j, pl.ds(base + m, PACK, stride=stride), :].astype(BF16)

    def correlate(src, dst, j, base, stride, order):
        for m in range(stride):
            dst[j, pl.ds(base + m, PACK, stride=stride), :] = products(
                (src[j, m + i], tap_s[j, k]) for i, k in enumerate(order)
            )

    forward = range(width)
    backward = range(edge, -1, -1)

    def spread_taps(j):
        for k in range(width):
            row = taps_ref[pl.ds(k, 1), cols(j)].astype(F32)
            tap_s[j, k] = jnp.broadcast_to(row, (PACK, LANES)).astype(BF16)

    def gate_tile(j):
        for base, size in (first_rows, *late):
            at = pl.ds(base, size)
            a = a_ref[at, cols(j)].astype(F32)
            g = g_ref[at, cols(j)].astype(F32)
            glu = a * jax.nn.sigmoid(g)
            if base == 0:
                glu = glu.astype(BF16).astype(F32)
            x_s[j, pl.ds(HALO + base, size), :] = glu
            if base + size == rows:
                glu_out[j] = glu[size - HALO :].astype(BF16)

    def far_tile(j):
        spread(x_s, xa_s, j, lead + HALO, far, far + edge)

    def gate_next(j, carry):
        far_tile(j - 1)
        gate_tile(j)
        return carry

    loads[0].wait()
    each_tile(spread_taps)
    for h in range(parts):
        loads[1 + 2 * h].wait()
        loads[2 + 2 * h].wait()
        if h == 0:
            gate_tile(0)
        lax.fori_loop(max(h * split, 1), (h + 1) * split, gate_next, 0)
    far_tile(tiles - 1)
    pl.semaphore_wait(barrier, n)

    @pl.when(me < n - 1)
    def _():
        glu_copy.start()

    each_tile(lambda j: correlate(xa_s, conv_s, j, HALO, far, forward))

    def stat_copy(phase, rows_of):
        at = pl.ds(*rows_of)
        return pltpu.make_async_remote_copy(
            src_ref=st_out.at[phase, :, at, :], dst_ref=st_in.at[phase, :, at, :],
            send_sem=st_send.at[0],
            recv_sem=st_recv.at[phase, ((0, HALO), *late).index(rows_of)],
            device_id={"tp": other},
        )

    def send_stats(phase, rows_of, first, second):
        st_out[phase, 0, pl.ds(*rows_of), :] = first
        st_out[phase, 1, pl.ds(*rows_of), :] = second
        stat_copy(phase, rows_of).start()

    def both_stats(group, phase):
        for rows_of in group:
            stat_copy(phase, rows_of).wait_recv()
        for rows_of in group:
            at = pl.ds(*rows_of)
            both = (st_out[phase, :, at, :] + st_in[phase, :, at, :]) * (1.0 / full)
            first, second = (
                jnp.broadcast_to(jnp.sum(both[q], axis=1, keepdims=True), both[q].shape)
                for q in range(2)
            )
            if phase == 0:
                second = lax.rsqrt(jnp.maximum(second - first * first, 0.0) + EPS)
            stat_s[2 * phase, at, :] = first
            stat_s[2 * phase + 1, at, :] = second

    def zeros(rows_of):
        zero = jnp.zeros((rows_of[1], LANES), F32)
        return zero, zero

    def moments(rows_of):
        def step(j, carry):
            first, second = carry
            x = conv_s[j, pl.ds(*rows_of), :]
            return first + x, second + x * x

        send_stats(0, rows_of, *over_tiles(step, zeros(rows_of), 3))

    def fold(x):
        return jnp.sum(x.reshape(x.shape[0] // SUB, SUB, LANES), axis=0)

    def normalise(rows_of):
        at = pl.ds(*rows_of)
        mean = stat_s[0, at, :]
        rstd = stat_s[1, at, :]

        def step(j, carry):
            first, second = carry
            gain = par_s[j, 0:1, :]
            normed = (conv_s[j, at, :] - mean) * rstd
            pre = normed * gain + par_s[j, 1:2, :]
            sig = jax.nn.sigmoid(pre)
            dpre = cot_ref[at, cols(j)].astype(F32) * sig * (1.0 + pre * (1.0 - sig))
            par_s[j, pl.ds(SUB, SUB), :] += fold(dpre * normed)
            par_s[j, pl.ds(2 * SUB, SUB), :] += fold(dpre)
            dn = dpre * gain
            conv_s[j, at, :] = normed
            dn_s[j, at, :] = dn
            return first + dn, second + dn * normed

        send_stats(1, rows_of, *over_tiles(step, zeros(rows_of), 1))

    def dconv(rows_of):
        at = pl.ds(*rows_of)
        rstd = stat_s[1, at, :]
        first = stat_s[2, at, :]
        second = stat_s[3, at, :]

        def step(j, carry):
            d_s[j, at, :] = rstd * (dn_s[j, at, :] - first - conv_s[j, at, :] * second)
            return carry

        over_tiles(step, 0, 2)

    for b in late:
        moments(b)

    loads[-3].wait()
    loads[-2].wait()

    def parameters(j):
        par_s[j, 0:1, :] = gain_ref[cols(j)].reshape(1, LANES)
        par_s[j, 1:2, :] = shift_ref[cols(j)].reshape(1, LANES)
        par_s[j, pl.ds(SUB, 2 * SUB), :] = jnp.zeros((2 * SUB, LANES), F32)
        part_s[j, pl.ds(width * STEP, (slots - width) * STEP), :] = jnp.zeros(
            ((slots - width) * STEP, LANES), F32
        )

    each_tile(parameters)
    loads[-1].wait()
    both_stats(late, 0)
    for b in late:
        normalise(b)

    @pl.when(me > 0)
    def _():
        glu_copy.wait_recv()

        def widen(j):
            x_s[j, pl.ds(0, HALO), :] = glu_in[j].astype(F32)

        each_tile(widen)

    @pl.when(me == 0)
    def _():
        def clear(j):
            x_s[j, pl.ds(0, HALO), :] = jnp.zeros((HALO, LANES), F32)

        each_tile(clear)

    def near_tile(j):
        spread(x_s, xb_s, j, lead, near, near + edge)
        correlate(xb_s, conv_s, j, 0, near, forward)

    each_tile(near_tile)
    moments(first_rows)
    both_stats(late, 1)
    for b in late:
        dconv(b)

    def taps_far(h):
        def step(i, carry):
            j = h * part_tiles + i
            spread(d_s, d_t, j, HALO, far, far)
            for k in range(width):
                both = products((xa_s[j, m + k], d_t[j, m]) for m in range(far))
                part_s[j, pl.ds(k * STEP, SUB), :] = both[:SUB] + both[SUB:]
            return carry

        lax.fori_loop(0, part_tiles, step, 0)

    spare = owners * chunk - part_tiles * (slots + 1)

    def taps_near(h):
        def step(i, carry):
            j = h * part_tiles + i
            d = [d_s[j, pl.ds(r, SUB), :] for r in range(0, HALO, SUB)]
            for k in range(width):
                total = part_s[j, pl.ds(k * STEP, SUB), :]
                for r in range(0, HALO, SUB):
                    total = total + d[r // SUB] * x_s[j, pl.ds(lead + k + r, SUB), :]
                part_s[j, pl.ds(k * STEP, SUB), :] = total
            part_s[j, pl.ds(width * STEP, SUB), :] = par_s[j, pl.ds(SUB, SUB), :]
            for q in range(slots // SUB):
                total = part_s[j, pl.ds(q * SUB * STEP, SUB, stride=STEP), :]
                for r in range(1, SUB):
                    total = total + part_s[j, pl.ds(q * SUB * STEP + r, SUB, stride=STEP), :]
                red_f[pl.ds(pl.multiple_of(i * slots, SUB) + q * SUB, SUB), :] = total
            red_f[pl.ds(part_tiles * slots + i, 1), :] = jnp.sum(
                par_s[j, pl.ds(2 * SUB, SUB), :], axis=0, keepdims=True
            )
            return carry

        lax.fori_loop(0, part_tiles, step, 0)
        if spare:
            red_f[pl.ds(part_tiles * (slots + 1), spare), :] = jnp.zeros((spare, LANES), F32)
        red_s[h] = red_f[...].astype(BF16)

    taps_far(0)
    both_stats((first_rows,), 0)
    normalise(first_rows)
    for h in range(1, rounds):
        taps_far(h)
    both_stats((first_rows,), 1)
    dconv(first_rows)

    mine = me - first_owner
    owner = jnp.logical_and(mine >= 0, mine < owners)

    def part(o):
        return pl.ds(pl.multiple_of(o * chunk, PACK), chunk)

    def bytes_of(ref, sem):
        return pltpu.make_async_copy(ref, ref, sem)

    def scatter(h):
        def step(i, carry):
            o = lax.rem(me + i, owners)
            to = first_owner + o

            @pl.when(to != me)
            def _():
                pltpu.make_async_remote_copy(
                    src_ref=red_s.at[h, part(o), :],
                    dst_ref=rs_in.at[h, lax.rem(me - to + n, n) - 1],
                    send_sem=rs_send.at[h], recv_sem=rs_recv.at[h], device_id={"sp": to},
                ).start()

            return carry

        lax.fori_loop(0, owners, step, 0)

    def gather(h):
        @pl.when(owner)
        def _():
            bytes_of(rs_in.at[h], rs_recv.at[h]).wait()
            ag_src[h] = lax.fori_loop(
                0, n - 1, lambda s, total: total + rs_in[h, s].astype(F32),
                red_s[h, part(mine), :].astype(F32),
            ).astype(BF16)

            def step(i, carry):
                pltpu.make_async_remote_copy(
                    src_ref=ag_src.at[h], dst_ref=ag_in.at[h, part(mine), :],
                    send_sem=ag_send.at[h], recv_sem=ag_recv.at[h],
                    device_id={"sp": lax.rem(me + i, n)},
                ).start()
                return carry

            lax.fori_loop(1, n, step, 0)

    for h in range(rounds):
        taps_near(h)
        scatter(h)

    def back_far(j):
        spread(d_s, da_s, j, 0, far, far + edge)
        correlate(da_s, x_s, j, 0, far, backward)

    def back_near(j):
        spread(d_s, db_s, j, rows - HALO, near, near + edge)
        correlate(db_s, x_s, j, rows - HALO, near, backward)

    def outputs(rows_of):
        at = pl.ds(*rows_of)

        def run(j):
            sig = jax.nn.sigmoid(g_ref[at, cols(j)].astype(F32))
            first = x_s[j, at, :] * sig
            ag_ref[at, cols(j)] = first.astype(BF16)
            gg_ref[at, cols(j)] = (first * a_ref[at, cols(j)].astype(F32) * (1.0 - sig)).astype(BF16)

        each_tile(run)

    def head(j):
        dc_out[j] = d_s[j, pl.ds(0, HALO), :].astype(BF16)

    each_tile(head)
    each_tile(back_far)
    for b in range(0, rows - HALO, BLOCK):
        outputs((b, min(BLOCK, rows - HALO - b)))

    @pl.when(me > 0)
    def _():
        dc_copy.start()

    for h in range(rounds):
        gather(h)

    @pl.when(me < n - 1)
    def _():
        dc_copy.wait_recv()

        def widen(j):
            d_s[j, pl.ds(rows, HALO), :] = dc_in[j].astype(F32)

        each_tile(widen)

    @pl.when(me == n - 1)
    def _():
        def clear(j):
            d_s[j, pl.ds(rows, HALO), :] = jnp.zeros((HALO, LANES), F32)

        each_tile(clear)

    each_tile(back_near)
    outputs((rows - HALO, HALO))

    @pl.when(me < n - 1)
    def _():
        glu_copy.wait_send()

    @pl.when(me > 0)
    def _():
        dc_copy.wait_send()

    bytes_of(stat_s, st_send.at[0]).wait()

    for h in range(rounds):
        @pl.when(owner)
        def _():
            bytes_of(rs_in.at[h], ag_send.at[h]).wait()
            if owners > 1:
                rest = pl.ds(0, (owners - 1) * chunk)
                bytes_of(red_s.at[h, rest, :], rs_send.at[h]).wait()
                bytes_of(ag_in.at[h, rest, :], ag_recv.at[h]).wait()
            ag_in[h, part(mine), :] = ag_src[h]

        @pl.when(jnp.logical_not(owner))
        def _():
            bytes_of(red_s.at[h], rs_send.at[h]).wait()
            bytes_of(ag_in.at[h], ag_recv.at[h]).wait()

        sums_ref[h] = ag_in[h].astype(F32)


def finish(
    width, slots, part_tiles,
    ag_ref, gg_ref, sums_ref,
    ag_out, gg_out, tg_out, gaing_out, shiftg_out,
    tg_ref, gaing_ref, shiftg_ref, sems,
):
    copies = [
        pltpu.make_async_copy(src, dst, sems.at[i])
        for i, (src, dst) in enumerate((
            (ag_ref, ag_out), (gg_ref, gg_out), (tg_ref, tg_out),
            (gaing_ref, gaing_out), (shiftg_ref, shiftg_out),
        ))
    ]
    copies[0].start()
    copies[1].start()
    for h in range(sums_ref.shape[0]):
        for i in range(part_tiles):
            at = pl.ds((h * part_tiles + i) * LANES, LANES)
            tg_ref[:, at] = sums_ref[h, pl.ds(i * slots, width), :]
            gaing_ref[at] = sums_ref[h, i * slots + width, :]
            shiftg_ref[at] = sums_ref[h, part_tiles * slots + i, :]
    for copy in copies[2:]:
        copy.start()
    for copy in copies:
        copy.wait()


def solution(mesh):
    n, ntp = mesh.shape["sp"], mesh.shape["tp"]

    def body(proj_a, proj_gate, taps, norm_gain, norm_shift, cotangent):
        rows, chans = proj_a.shape
        width = taps.shape[0]
        edge = width - 1
        tiles, rounds, slots, chunk, owners, _ = plan(chans, width, n)
        blocks = 1 + rows // BLOCK
        far, near = (rows - HALO) // PACK, HALO // PACK
        vmem = pl.BlockSpec(memory_space=pltpu.VMEM)
        hbm = pl.BlockSpec(memory_space=pltpu.HBM)
        wide = jax.ShapeDtypeStruct((rows, chans), BF16)
        a_grad, gate_grad, sums = pl.pallas_call(
            functools.partial(kernel, n, width, chans * ntp),
            out_shape=(wide, wide, jax.ShapeDtypeStruct((rounds, owners * chunk, LANES), F32)),
            in_specs=[hbm] * 6,
            out_specs=(vmem,) * 3,
            scratch_shapes=[
                pltpu.VMEM((rows, chans), BF16),
                pltpu.VMEM((rows, chans), BF16),
                pltpu.VMEM((rows, chans), BF16),
                pltpu.VMEM((width, chans), BF16),
                pltpu.VMEM((chans,), F32),
                pltpu.VMEM((chans,), F32),
                pltpu.VMEM((tiles, width, PACK, LANES), BF16),
                pltpu.VMEM((tiles, HALO + rows, LANES), F32),
                pltpu.VMEM((tiles, far + edge, PACK, LANES), BF16),
                pltpu.VMEM((tiles, near + edge, PACK, LANES), BF16),
                pltpu.VMEM((tiles, rows, LANES), F32),
                pltpu.VMEM((tiles, rows, LANES), F32),
                pltpu.VMEM((tiles, rows + HALO, LANES), F32),
                pltpu.VMEM((tiles, far, PACK, LANES), BF16),
                pltpu.VMEM((tiles, far + edge, PACK, LANES), BF16),
                pltpu.VMEM((tiles, near + edge, PACK, LANES), BF16),
                pltpu.VMEM((tiles, 3 * SUB, LANES), F32),
                pltpu.VMEM((tiles, slots * STEP, LANES), F32),
                pltpu.VMEM((tiles, HALO, LANES), BF16),
                pltpu.VMEM((tiles, HALO, LANES), BF16),
                pltpu.VMEM((tiles, HALO, LANES), BF16),
                pltpu.VMEM((tiles, HALO, LANES), BF16),
                pltpu.VMEM((2, 2, rows, LANES), F32),
                pltpu.VMEM((2, 2, rows, LANES), F32),
                pltpu.VMEM((4, rows, LANES), F32),
                pltpu.VMEM((owners * chunk, LANES), F32),
                pltpu.VMEM((rounds, owners * chunk, LANES), BF16),
                pltpu.VMEM((rounds, n - 1, chunk, LANES), BF16),
                pltpu.VMEM((rounds, chunk, LANES), BF16),
                pltpu.VMEM((rounds, owners * chunk, LANES), BF16),
                pltpu.SemaphoreType.DMA((8,)),
                pltpu.SemaphoreType.DMA((2,)),
                pltpu.SemaphoreType.DMA((2,)),
                pltpu.SemaphoreType.DMA((1,)),
                pltpu.SemaphoreType.DMA((2, blocks)),
                pltpu.SemaphoreType.DMA((rounds,)),
                pltpu.SemaphoreType.DMA((rounds,)),
                pltpu.SemaphoreType.DMA((rounds,)),
                pltpu.SemaphoreType.DMA((rounds,)),
            ],
            compiler_params=pltpu.CompilerParams(
                collective_id=0, has_side_effects=True, vmem_limit_bytes=40 * 1024 * 1024
            ),
        )(*(
            pltpu.with_memory_space_constraint(x, pltpu.HBM)
            for x in (proj_a, proj_gate, taps, norm_gain, norm_shift, cotangent)
        ))
        vector = jax.ShapeDtypeStruct((chans,), F32)
        return pl.pallas_call(
            functools.partial(finish, width, slots, tiles // rounds),
            out_shape=(wide, wide, jax.ShapeDtypeStruct((width, chans), F32), vector, vector),
            in_specs=[vmem] * 3,
            out_specs=(hbm,) * 5,
            scratch_shapes=[
                pltpu.VMEM((width, chans), F32),
                pltpu.VMEM((chans,), F32),
                pltpu.VMEM((chans,), F32),
                pltpu.SemaphoreType.DMA((5,)),
            ],
            compiler_params=pltpu.CompilerParams(vmem_limit_bytes=16 * 1024 * 1024),
        )(a_grad, gate_grad, sums)

    placed = (P("sp", "tp"), P("sp", "tp"), P(None, "tp"), P("tp"), P("tp"), P("sp", "tp"))
    return jax.shard_map(
        body,
        mesh=mesh,
        in_specs=placed,
        out_specs=(P("sp", "tp"), P("sp", "tp"), P(None, "tp"), P("tp"), P("tp")),
        check_vma=False,
    )
```
